32 devices in a mesh: rep: 2 (over x), fs: 8 (over z, y), tp: 2 (over core).
Axes of the slice: x: 2, y: 2, z: 4, core: 2. Of those that a mesh axis runs over, the one named last changes fastest.
Arguments:
- inputs: bfloat16 [4096, 2048], P(('rep', 'fs')), may hold values from -6 to 6
- cotangent: bfloat16 [4096, 2048], P(('rep', 'fs')), may hold values from -0.119628906 to 0.119628906
- up_weight: bfloat16 [2048, 4096], P('fs', 'tp'), may hold values from -0.125 to 0.125
- down_weight: bfloat16 [4096, 2048], P('tp', 'fs'), may hold values from -0.09375 to 0.09375
Outputs:
- grad_inputs: float32 [4096, 2048], P(('rep', 'fs'))
- grad_up: float32 [2048, 4096], P('fs', 'tp')
- grad_down: float32 [4096, 2048], P('tp', 'fs')
- norms_up: float32 [2048], P('fs')
- norms_down: float32 [4096], P('tp')
The draws below stay inside these ranges and needn't reach their ends.
All inputs are finite; a program needn't handle non-finite values.
Results may differ from the reference program's by a relative error of at most 0.0029.
Values may be sent and summed in bfloat16 or wider, within the bound.
No kernel may reach another device: no remote copies, remote signals or barrier semaphores. Data moves between devices by JAX's collectives and lax.ppermute only.
A program may use at most 128 MiB of HBM per device.

```python
import jax
import jax.numpy as jnp
from jax import lax

D = 2048
FF = 4096
TOKENS = 4096


def spiked(array, rng, source, target, parts, factor):
    owner, partner = [(jnp.arange(array.shape[dim]) // (array.shape[dim] // parts)).reshape([-1 if axis == dim else 1 for axis in range(array.ndim)]) for dim in (source, target)]
    chosen = jax.random.permutation(rng, parts)[partner]
    strong = (owner == chosen) | (owner == (partner + parts // 2) % parts)
    return jnp.where(strong, factor * array, array)


def block_scale(own_key, shape, pieces, low, largest):
    def one(axis_at, shards_of):
        draws = jax.random.uniform(jax.random.fold_in(jax.random.fold_in(own_key, 6), axis_at), (shards_of,), jnp.float32, low / len(pieces), largest / len(pieces))
        return jnp.repeat(jnp.exp(draws), shape[axis_at] // shards_of).reshape((-1,) + (1,) * (len(shape) - axis_at - 1))

    level = one(*pieces[0])
    for cut in pieces[1:]:
        level = level * one(*cut)
    return level


def gaussian(rng, shape, spread, bound, pieces=(), held_as=jnp.bfloat16):
    array = spread * jax.random.normal(rng, shape, jnp.float32)
    if pieces:
        array = array * block_scale(rng, shape, pieces, -0.22, 0.18)
    return jnp.clip(array, -bound, bound).astype(held_as)


def noise_with(stream_key, shape, scale, bound, split, heavy, held_as=jnp.bfloat16):
    result = scale * jax.random.normal(stream_key, shape, jnp.float32)
    if split:
        result = result * block_scale(stream_key, shape, split, -0.22, 0.18)
    return jnp.clip(spiked(result, jax.random.fold_in(stream_key, 3), *heavy), -bound, bound).astype(held_as)


def setup_inputs(seed: int = 0) -> dict:
    arg_keys = jax.random.split(jax.random.key(seed), 5)
    return {
        "inputs": noise_with(arg_keys[0], (TOKENS, D), 1.0, 6.0, ((0, 16),), (0, 1, 16, 2.0)),
        "cotangent": noise_with(arg_keys[1], (TOKENS, D), 0.02, 0.119628906, ((0, 16),), (0, 1, 16, 2.0)),
        "up_weight": gaussian(arg_keys[2], (D, FF), D ** -0.5, 0.125, ((0, 8), (1, 2))),
        "down_weight": gaussian(arg_keys[3], (FF, D), FF ** -0.5, 0.09375, ((0, 2), (1, 8))),
    }


def contract(left, right, left_dim, right_dim):
    return lax.dot_general(left, right, (((left_dim,), (right_dim,)), ((), ())), preferred_element_type=jnp.float32)


def reference(inputs, cotangent, up_weight, down_weight):
    pre_act = jnp.dot(inputs, up_weight, preferred_element_type=jnp.float32)
    rectified = jnp.maximum(pre_act, 0.0)
    hidden = (rectified * rectified).astype(jnp.bfloat16)
    act_grad = contract(cotangent, down_weight, 1, 1)
    pre_grad = (2.0 * rectified * act_grad).astype(jnp.bfloat16)
    grad_down = contract(hidden, cotangent, 0, 0)
    grad_up = contract(inputs, pre_grad, 0, 0)
    grad_inputs = contract(pre_grad, up_weight, 1, 1)
    norms_up = jnp.sum(grad_up * grad_up, axis=1)
    norms_down = jnp.sum(grad_down * grad_down, axis=1)
    return (grad_inputs, grad_up, grad_down, norms_up, norms_down)
```

```python
import math

import jax
import jax.numpy as jnp
from jax import lax
from jax.sharding import Mesh, PartitionSpec as P


def dot(left, right, left_dim, right_dim):
    return lax.dot_general(
        left, right, (((left_dim,), (right_dim,)), ((), ())), preferred_element_type=jnp.float32
    )


def gather(x, axis, size):
    if size == 1:
        return x[None]
    if size != 2:
        return lax.all_gather(x, axis, axis=0)
    other = lax.ppermute(x, axis, [(0, 1), (1, 0)])
    first = lax.axis_index(axis) == 0
    return jnp.stack([jnp.where(first, x, other), jnp.where(first, other, x)])


def scatter_sum(x, axis, size, sent):
    if size == 1:
        return x[0]
    place = lax.axis_index(axis)
    if size == 2:
        theirs = lax.dynamic_index_in_dim(x, 1 - place, 0, keepdims=False)
        mine = lax.dynamic_index_in_dim(x, place, 0, keepdims=False)
        got = lax.ppermute(theirs.astype(sent), axis, [(0, 1), (1, 0)])
        return mine + got.astype(jnp.float32)
    got = lax.all_to_all(x.astype(sent), axis, 0, 0)
    return jnp.sum(got.astype(jnp.float32), axis=0)


def line_gather(x, axis, size, beside):
    ups, downs = [x], [x]
    for step in range(1, size):
        if step == 2:
            ups[-1], downs[-1], beside = lax.optimization_barrier((ups[-1], downs[-1], beside))
        ups.append(lax.ppermute(ups[-1], axis, [(j, j + 1) for j in range(step - 1, size - 1)]))
        downs.append(lax.ppermute(downs[-1], axis, [(j + 1, j) for j in range(size - step)]))
    place = lax.axis_index(axis)
    slots = [jnp.where(place >= d, ups[d], downs[size - d]) for d in range(1, size)]
    return jnp.concatenate([x] + slots, axis=0), beside


def all_sum(x, axes):
    for axis, size in axes:
        if size & (size - 1):
            x = lax.psum(x, axis)
            continue
        bit = 1
        while bit < size:
            x = x + lax.ppermute(x, axis, [(j, j ^ bit) for j in range(size)])
            bit *= 2
    return x


def return_sum(x, axis, size):
    total = x[0].astype(jnp.float32)
    for d in range(1, size):
        pairs = [(j, (j - d) % size) for j in range(size)]
        total = total + lax.ppermute(x[d], axis, pairs).astype(jnp.float32)
    return total


def solution(mesh):
    sizes = dict(mesh.shape)
    rep, fs, tp = sizes["rep"], sizes["fs"], sizes["tp"]
    far = math.gcd(4, fs)
    near = fs // far
    grid = Mesh(mesh.devices.reshape(rep, far, near, tp), ("rep", "far", "near", "tp"))

    def shards(inputs, cotangent, up_weight, down_weight):
        tokens, width = inputs.shape
        rows, hidden_own = up_weight.shape
        cut = hidden_own // far
        both = 2 * width // tp
        bf16 = jnp.bfloat16

        weights = jnp.stack([up_weight, down_weight.T]).reshape(2, rows, far, cut)
        half = rows // rep
        weights = weights.transpose(2, 0, 1, 3)
        weights = lax.dynamic_slice_in_dim(weights, lax.axis_index("rep") * half, half, 2)
        weights = lax.all_to_all(weights, "far", 0, 0)

        place = lax.axis_index("tp")
        joined = jnp.concatenate([inputs, cotangent], axis=1)
        share = lax.dynamic_slice_in_dim(joined, place * both, both, 1)
        share, weights = lax.optimization_barrier((share, weights))
        share, weights = line_gather(share, "far", far, gather(weights, "rep", rep))
        weights = gather(weights, "near", near).transpose(3, 2, 0, 1, 4, 5)
        weights = weights.reshape(2, width, cut)
        up, down = weights[0], weights[1]
        share = gather(share, "tp", tp)
        if tp == 2:
            x, c = share[0], share[1]
        else:
            whole = share.transpose(1, 0, 2).reshape(far * tokens, 2 * width)
            x, c = whole[:, :width], whole[:, width:]

        rectified = jnp.maximum(dot(x, up, 1, 0), 0.0)
        hidden = (rectified * rectified).astype(bf16)
        pre_grad = (2.0 * rectified * dot(c, down, 1, 0)).astype(bf16)

        def finish(grad):
            grad = grad.reshape(far, near, rows, cut).transpose(1, 0, 2, 3)
            grad = scatter_sum(grad, "near", near, bf16)
            grad = grad.reshape(far, rep, half, cut).transpose(1, 0, 2, 3)
            grad = scatter_sum(grad, "rep", rep, bf16)
            grad = lax.all_to_all(grad.astype(bf16), "far", 0, 0)
            grad = gather(grad, "rep", rep).astype(jnp.float32)
            return grad.transpose(0, 2, 1, 3).reshape(rows, hidden_own)

        back = dot(pre_grad, up, 1, 1).reshape(far * tokens, tp, width // tp)
        back = scatter_sum(back.transpose(1, 0, 2), "tp", tp, jnp.float32)
        back = back.reshape(far, tokens, width // tp).astype(bf16)
        down_turned = finish(dot(c, hidden, 0, 0))
        back, pre_grad = lax.optimization_barrier((back, pre_grad))
        grad_up = finish(dot(x, pre_grad, 0, 0))
        norms_down = jnp.sum(down_turned * down_turned, axis=0)
        norms_down = all_sum(norms_down, (("near", near), ("far", far)))
        norms_up = all_sum(jnp.sum(grad_up * grad_up, axis=1), (("tp", tp),))

        back = return_sum(back, "far", far)
        back = gather(back, "tp", tp)
        grad_inputs = back.transpose(1, 0, 2).reshape(tokens, width)
        return grad_inputs, grad_up, down_turned.T, norms_up, norms_down

    fsa = ("far", "near")
    return jax.shard_map(
        shards,
        mesh=grid,
        in_specs=(P(("rep",) + fsa, None), P(("rep",) + fsa, None), P(fsa, "tp"), P("tp", fsa)),
        out_specs=(P(("rep",) + fsa, None), P(fsa, "tp"), P("tp", fsa), P(fsa), P("tp")),
        check_vma=False,
    )
```
